32 devices in a mesh: sp: 4 (over z), dp: 8 (over y, x, core).
Axes of the slice: x: 2, y: 2, z: 4, core: 2. Of those that a mesh axis runs over, the one named last changes fastest.
Arguments:
- tokens: bfloat16 [8, 512, 2048], P('dp', 'sp'), may hold values from -6 to 6
- receptance_weight: bfloat16 [2048, 1024], P('dp'), may hold values from -0.125 to 0.125
- key_projection_weight: bfloat16 [2048, 1024], P('dp'), may hold values from -0.125 to 0.125
- value_projection_weight: bfloat16 [2048, 1024], P('dp'), may hold values from -0.125 to 0.125
- decay_down_weight: bfloat16 [2048, 256], P('dp'), may hold values from -0.125 to 0.125
- decay_up_weight: bfloat16 [2, 128, 1024], replicated, may hold values from -0.71875 to 0.71875
- decay_floor_level: float32 [2, 1024], replicated, may hold values from -10 to -2.25
- correction_rate_logit: float32 [2, 1024], P(None, 'sp'), may hold values from -4 to 4
- diagonal_address_factor: float32 [2, 1024], P(None, 'sp'), may hold values from -1 to 1
- head_norm_gain: float32 [1024], P('sp'), may hold values from 0.1 to 1.9
Outputs:
- mixed: bfloat16 [8, 512, 1024], P('dp', 'sp')
The draws below stay inside these ranges and needn't reach their ends.
All inputs are finite; a program needn't handle non-finite values.
Results may differ from the reference program's by a relative error of at most 0.0056.
The reference program's roundings to bfloat16 on the way (of `lowered` and `pre`) count: a program that leaves them out, or rounds other values in their place, can miss the bound.
Values may be sent and summed in bfloat16 or wider, within the bound.
A program may use at most 128 MiB of HBM per device.

```python
import math
import jax
import jax.numpy as jnp
from jax import lax

D = 2048
ATTENTION_SPLITS = 16
SUBSPACE_SIZE = 64
RANK = 128
CHANNEL_COUNT = 1024
LENGTH = 512
SEQS = 8


def draw_decay_floor_level(key, part):
    first, second, third, fourth = jax.random.split(key, 4)
    keep = 5
    slow = jax.random.randint(first, (2, ATTENTION_SPLITS, 1), 0, 10) < keep
    slow_level = jax.random.uniform(second, (2, ATTENTION_SPLITS, 1), jnp.float32, -9.5, -8.5)
    fast_level = jax.random.uniform(third, (2, ATTENTION_SPLITS, 1), jnp.float32, -3.25, -2.75)
    jitter = jax.random.uniform(fourth, (2, ATTENTION_SPLITS, SUBSPACE_SIZE), jnp.float32, -0.5, 0.5)
    return (jnp.where(slow, slow_level, fast_level) + jitter).reshape(2, ATTENTION_SPLITS * SUBSPACE_SIZE)


def level_of(stream_key, shape, cuts, low, high):
    loudness = 1.0
    for axis_at, parts in cuts:
        heights = jax.random.uniform(jax.random.fold_in(jax.random.fold_in(stream_key, 6), axis_at), (parts,), jnp.float32, low / len(cuts), high / len(cuts))
        loudness = loudness * jnp.repeat(jnp.exp(heights), shape[axis_at] // parts).reshape((-1,) + (1,) * (len(shape) - 1 - axis_at))
    return loudness


def gaussian(own_key, dims, scale, limit, cuts=(), dtype=jnp.bfloat16):
    entries = scale * jax.random.normal(own_key, dims, jnp.float32)
    if cuts:
        entries = entries * level_of(own_key, dims, cuts, -0.22, 0.18)
    return jnp.clip(entries, -limit, limit).astype(dtype)


def setup_inputs(seed: int = 0) -> dict:
    splits = jax.random.split(jax.random.key(seed), 11)
    tokens = gaussian(splits[0], (SEQS, LENGTH, D), 1.0, 6.0, ((0, 8), (1, 4)))
    receptance_weight = gaussian(splits[1], (D, CHANNEL_COUNT), D ** -0.5, 0.125, ((0, 8),))
    key_projection_weight = gaussian(splits[2], (D, CHANNEL_COUNT), D ** -0.5, 0.125, ((0, 8),))
    value_projection_weight = gaussian(splits[3], (D, CHANNEL_COUNT), D ** -0.5, 0.125, ((0, 8),))
    decay_down_weight = gaussian(splits[4], (D, 2 * RANK), D ** -0.5, 0.125, ((0, 8),))
    decay_up_weight = gaussian(splits[5], (2, RANK, CHANNEL_COUNT), 0.12, 0.71875)
    decay_floor_level = draw_decay_floor_level(jax.random.fold_in(splits[10], 71), 0)
    correction_rate_logit = gaussian(splits[7], (2, CHANNEL_COUNT), 1.0, 4.0, ((1, 4),), jnp.float32)
    diagonal_address_factor = gaussian(splits[8], (2, CHANNEL_COUNT), 0.2, 1.0, ((1, 4),), jnp.float32)
    head_norm_gain = jnp.clip(1.0 + 0.18 * jax.random.normal(splits[9], (CHANNEL_COUNT,), jnp.float32), 0.1, 1.9)
    return {"tokens": tokens, "receptance_weight": receptance_weight, "key_projection_weight": key_projection_weight, "value_projection_weight": value_projection_weight, "decay_down_weight": decay_down_weight, "decay_up_weight": decay_up_weight, "decay_floor_level": decay_floor_level, "correction_rate_logit": correction_rate_logit, "diagonal_address_factor": diagonal_address_factor, "head_norm_gain": head_norm_gain}


def contract(pattern, former, latter):
    return jnp.einsum(pattern, former, latter, precision=lax.Precision.HIGHEST)

def recur(state, inputs):
    query, rated_key, value, eraser, writer, decay = inputs
    pulled = contract('hij,hj->hi', state, eraser)
    state = state * decay[:, None, :] + pulled[:, :, None] * writer[:, None, :] + value[:, :, None] * rated_key[:, None, :]
    return (state, contract('hij,hj->hi', state, query))

def reference(tokens, receptance_weight, key_projection_weight, value_projection_weight, decay_down_weight, decay_up_weight, decay_floor_level, correction_rate_logit, diagonal_address_factor, head_norm_gain):
    flat = tokens.reshape(SEQS * LENGTH, D)
    receive = jnp.dot(flat, receptance_weight, preferred_element_type=jnp.float32).astype(jnp.bfloat16)
    key_rows = jnp.dot(flat, key_projection_weight, preferred_element_type=jnp.float32).astype(jnp.bfloat16)
    value_rows = jnp.dot(flat, value_projection_weight, preferred_element_type=jnp.float32).astype(jnp.bfloat16)
    lowered = jnp.tanh(jnp.dot(flat, decay_down_weight, preferred_element_type=jnp.float32)).astype(jnp.bfloat16)
    forward_pre = (jnp.dot(lowered[:, :RANK], decay_up_weight[0], preferred_element_type=jnp.float32) + decay_floor_level[0]).astype(jnp.bfloat16)
    backward_pre = (jnp.dot(lowered[:, RANK:], decay_up_weight[1], preferred_element_type=jnp.float32) + decay_floor_level[1]).astype(jnp.bfloat16)
    amend_strength = jax.nn.sigmoid(correction_rate_logit).reshape(2, ATTENTION_SPLITS, SUBSPACE_SIZE)
    diagonal_extra = diagonal_address_factor.reshape(2, ATTENTION_SPLITS, SUBSPACE_SIZE)
    gain = head_norm_gain.reshape(ATTENTION_SPLITS, SUBSPACE_SIZE)

    def to_sequences(content_matrix_full):
        return content_matrix_full.reshape(SEQS, LENGTH, ATTENTION_SPLITS, SUBSPACE_SIZE)

    def one_sequence(items):
        probe_matrix_full, keys, content_matrix_full, fore, backs = [piece.astype(jnp.float32) for piece in items]
        normed = keys / jnp.sqrt(lax.optimization_barrier(jnp.sum(keys * keys, -1, keepdims=True)) + 1.0)
        total = jnp.zeros((LENGTH, ATTENTION_SPLITS, SUBSPACE_SIZE), jnp.float32)
        for sweep_orientation, pre in ((0, fore), (1, backs)):
            decay = jnp.exp(-math.exp(-0.5) * jax.nn.sigmoid(pre))
            strength_multiplied = keys * amend_strength[sweep_orientation]
            inputs = (probe_matrix_full, strength_multiplied, content_matrix_full, -normed, normed * amend_strength[sweep_orientation], decay)
            if sweep_orientation == 1:
                inputs = tuple((jnp.flip(piece, 0) for piece in inputs))
            state = jnp.zeros((ATTENTION_SPLITS, SUBSPACE_SIZE, SUBSPACE_SIZE), jnp.float32)
            _, readout = lax.scan(recur, state, inputs)
            if sweep_orientation == 1:
                readout = jnp.flip(readout, 0)
            centred = readout - lax.optimization_barrier(jnp.mean(readout, -1, keepdims=True))
            variance = lax.optimization_barrier(jnp.mean(centred * centred, -1, keepdims=True))
            diagonal_contribution = lax.optimization_barrier(jnp.sum(probe_matrix_full * strength_multiplied * diagonal_extra[sweep_orientation], -1, keepdims=True)) * content_matrix_full
            total = total + (centred * lax.rsqrt(variance + 0.00064) * gain + diagonal_contribution)
        return total.reshape(LENGTH, ATTENTION_SPLITS * SUBSPACE_SIZE).astype(jnp.bfloat16)
    return lax.map(one_sequence, (to_sequences(receive), to_sequences(key_rows), to_sequences(value_rows), to_sequences(forward_pre), to_sequences(backward_pre)))
```

```python
import functools
import math

import jax
import jax.numpy as jnp
from jax import lax
from jax.experimental import pallas as pl
from jax.experimental.pallas import tpu as pltpu
from jax.sharding import PartitionSpec as P

HEAD = 64
SPAN = 64
BF = jnp.bfloat16
F32 = jnp.float32
NT = (((1,), (1,)), ((), ()))
TN = (((0,), (0,)), ((), ()))


def mm(a, b):
    return jnp.dot(a, b, preferred_element_type=F32)


def split(x):
    hi = x.astype(BF)
    return hi, (x - hi.astype(F32)).astype(BF)


def iota(shape, axis):
    return lax.broadcasted_iota(jnp.int32, shape, axis)


def core_kernel(
    tok_ref, w_ref, up_ref, floor_ref, rate_ref, diag_ref, gain_ref, out_ref,
    eq_s, wp_s, qe_s, kend_s, cv_s, own_s, decay_s, diag_s, t_s, b_s, state_s, y_s,
):
    length, chans = out_ref.shape
    heads = chans // HEAD
    rank = up_ref.shape[1]
    rows = min(256, length)
    spans = rows // SPAN
    blocks = length // SPAN

    def head_ones():
        return (iota((chans, chans), 0) // HEAD == iota((chans, chans), 1) // HEAD).astype(BF)

    def head_sum(x, ones):
        hi, lo = split(x)
        return mm(hi, ones) + mm(lo, ones)

    @pl.loop(0, length // rows)
    def _(step):
        at = pl.ds(pl.multiple_of(step * rows, rows), rows)
        source = tok_ref[at, :]
        pr = mm(source, w_ref[:, :chans]).astype(BF).astype(F32)
        pk = mm(source, w_ref[:, chans : 2 * chans]).astype(BF).astype(F32)
        pv = mm(source, w_ref[:, 2 * chans : 3 * chans]).astype(BF).astype(F32)
        lowered = jnp.tanh(mm(source, w_ref[:, 3 * chans :])).astype(BF)
        ones = head_ones()
        norm2 = head_sum(pk * pk, ones) + 1.0
        inv = lax.rsqrt(norm2)
        scale = norm2 * inv
        normed = pk * inv
        cv_s[at, :] = scale * pv
        rates = jax.nn.sigmoid(rate_ref[...])
        both = jnp.sum(rates * diag_ref[...], axis=0, keepdims=True)
        own_s[at, :] = head_sum(pr * pk * both, ones) * pv
        ri = iota((rows, rows), 0)
        ci = iota((rows, rows), 1)
        same = ri // SPAN == ci // SPAN
        whole = same.astype(BF)
        for d in range(2):
            pre = (
                mm(lowered[:, d * rank : (d + 1) * rank], up_ref[d]) + floor_ref[d : d + 1, :]
            ).astype(BF).astype(F32)
            fall = -math.exp(-0.5) * jax.nn.sigmoid(pre)
            tri = jnp.logical_and(same, (ci <= ri) if d == 0 else (ci >= ri)).astype(BF)
            hi, lo = split(fall)
            inclusive = mm(tri, hi) + mm(tri, lo)
            final = mm(whole, hi) + mm(whole, lo)
            half = 0.5 * final
            grow = jnp.exp(inclusive - half)
            shrink = jnp.exp(half - inclusive)
            g = jnp.exp(half)
            e = -normed * (grow * jnp.exp(-fall))
            q = pr * grow
            w = normed * rates[d : d + 1, :] * shrink
            wp_s[d, at, :] = w.astype(BF)
            kend_s[d, at, :] = (w * g).astype(BF)
            eb, qb = e.astype(BF), q.astype(BF)
            eg, qg = (e * g).astype(BF), (q * g).astype(BF)
            g2 = g * g
            diag_s[d, at, :] = head_sum(pr * normed * rates[d : d + 1, :], ones)
            for s in range(spans):
                cut = slice(s * SPAN, (s + 1) * SPAN)
                base = pl.multiple_of((step * spans + s) * 2 * SPAN, 2 * SPAN)
                eq_s[d, pl.ds(base, SPAN), :] = eb[cut]
                eq_s[d, pl.ds(base + SPAN, SPAN), :] = qb[cut]
                qe_s[d, pl.ds(base, SPAN), :] = eg[cut]
                qe_s[d, pl.ds(base + SPAN, SPAN), :] = qg[cut]
                decay_s[d, pl.ds(pl.multiple_of((step * spans + s) * 8, 8), 8), :] = g2[
                    s * SPAN : s * SPAN + 8
                ]

    def spread(x, mask):
        x = x.astype(BF)
        if heads > 1:
            x = jnp.concatenate([x] * heads, axis=0)
        return x * mask

    group = 2 if blocks % 2 == 0 else 1

    @pl.loop(0, blocks // group)
    def _(step):
        mask = head_ones()
        ti = iota((SPAN, chans), 0)
        ji = iota((SPAN, chans), 1) % HEAD
        eye = (ti == ji).astype(F32)
        work = []
        for s in range(group):
            for d in range(2):
                block = step * group + s
                two = pl.ds(pl.multiple_of(block * 2 * SPAN, 2 * SPAN), 2 * SPAN)
                at = pl.ds(pl.multiple_of(block * SPAN, SPAN), SPAN)
                ab = lax.dot_general(
                    eq_s[d, two, :], spread(wp_s[d, at, :], mask), NT, preferred_element_type=F32
                )
                strict = (ti > ji) if d == 0 else (ti < ji)
                b_s[d, at, :] = jnp.where(strict, ab[SPAN:], 0.0).astype(BF)
                work.append((d, at, jnp.where(strict, ab[:SPAN], 0.0)))
        near = ti // 4 == ji // 4
        full = [a for _, _, a in work]
        base = [jnp.where(near, a, 0.0) for a in full]
        square = [mm(a.astype(BF), spread(a, mask)) for a in base]
        inverse = [eye + a for a in base]
        inverse = [t + mm(t.astype(BF), spread(a2, mask)) for t, a2 in zip(inverse, square)]
        size = 4
        while size < SPAN:
            far = jnp.logical_and(ti // (2 * size) == ji // (2 * size), ti // size != ji // size)
            first = [
                mm(t.astype(BF), spread(jnp.where(far, a, 0.0), mask))
                for t, a in zip(inverse, full)
            ]
            inverse = [t + mm(f.astype(BF), spread(t, mask)) for t, f in zip(inverse, first)]
            size *= 2
        for (d, at, _), t in zip(work, inverse):
            t_s[d, at, :] = (t - eye).astype(BF)

    state_s[...] = jnp.zeros_like(state_s)

    @pl.loop(0, blocks)
    def _(step):
        mask = head_ones()
        for d in range(2):
            block = step if d == 0 else blocks - 1 - step
            two = pl.ds(pl.multiple_of(block * 2 * SPAN, 2 * SPAN), 2 * SPAN)
            at = pl.ds(pl.multiple_of(block * SPAN, SPAN), SPAN)
            state = state_s[d]
            read = lax.dot_general(
                qe_s[d, two, :], state.astype(BF), NT, preferred_element_type=F32
            )
            x = cv_s[at, :] + read[:SPAN]
            exact = x + mm(t_s[d, at, :], spread(x, mask))
            a = exact.astype(BF)
            y_s[d, at, :] = read[SPAN:] + mm(b_s[d, at, :], spread(a, mask)) + diag_s[d, at, :] * exact
            decay = decay_s[d, pl.ds(pl.multiple_of(block * 8, 8), 8), :][:1]
            put = lax.dot_general(a, kend_s[d, at, :], TN, preferred_element_type=F32)
            state_s[d] = state * decay + put * mask.astype(F32)

    @pl.loop(0, length // rows)
    def _(step):
        at = pl.ds(pl.multiple_of(step * rows, rows), rows)
        ones = head_ones()
        total = own_s[at, :]
        for d in range(2):
            y = y_s[d, at, :]
            centred = y - head_sum(y, ones) * (1.0 / HEAD)
            variance = head_sum(centred * centred, ones) * (1.0 / HEAD)
            total = total + centred * lax.rsqrt(variance + 0.00064) * gain_ref[...]
        out_ref[at, :] = total.astype(BF)


def core_call(length, chans, interpret=False):
    vm = pltpu.VMEM
    both = lambda n, dt: vm((2, n, chans), dt)
    return pl.pallas_call(
        core_kernel,
        out_shape=jax.ShapeDtypeStruct((length, chans), BF),
        in_specs=[pl.BlockSpec(memory_space=vm)] * 7,
        out_specs=pl.BlockSpec(memory_space=vm),
        scratch_shapes=[
            both(2 * length, BF), both(length, BF), both(2 * length, BF), both(length, BF),
            vm((length, chans), F32), vm((length, chans), F32),
            both(length // SPAN * 8, F32), both(length, F32), both(length, BF), both(length, BF),
            vm((2, chans, chans), F32), both(length, F32),
        ],
        compiler_params=pltpu.CompilerParams(vmem_limit_bytes=56 * 1024 * 1024),
        interpret=interpret,
        name="core",
    )


def per_device(
    sp,
    tokens, receptance_weight, key_projection_weight, value_projection_weight,
    decay_down_weight, decay_up_weight, decay_floor_level, correction_rate_logit,
    diagonal_address_factor, head_norm_gain,
):
    rows, depth = tokens.shape[1:]
    channels = receptance_weight.shape[1]
    chans = channels // sp
    start = lax.axis_index("sp") * chans

    def mine(x):
        return lax.dynamic_slice_in_dim(x, start, chans, axis=x.ndim - 1)

    packed = jnp.concatenate(
        [mine(receptance_weight), mine(key_projection_weight), mine(value_projection_weight),
         decay_down_weight], axis=1)
    weights = lax.all_gather(packed, "dp", axis=0, tiled=True)
    source = lax.all_gather(tokens[0], "sp", axis=0, tiled=True)
    mixed = core_call(rows * sp, chans)(
        source, weights, mine(decay_up_weight), mine(decay_floor_level),
        correction_rate_logit, diagonal_address_factor, head_norm_gain[None, :])
    returned = lax.all_to_all(mixed, "sp", split_axis=0, concat_axis=1, tiled=True)
    return returned[None]


def solution(mesh):
    in_specs = (
        P("dp", "sp", None), P("dp", None), P("dp", None), P("dp", None), P("dp", None),
        P(), P(), P(None, "sp"), P(None, "sp"), P("sp"),
    )
    return jax.shard_map(
        functools.partial(per_device, mesh.shape["sp"]), mesh=mesh, in_specs=in_specs,
        out_specs=P("dp", "sp", None), check_vma=False,
    )
```

```python
import functools
import math

import jax
import jax.numpy as jnp
from jax import lax
from jax.experimental import pallas as pl
from jax.experimental.pallas import tpu as pltpu
from jax.sharding import PartitionSpec as P

HEAD = 64
SPAN = 64
BF = jnp.bfloat16
F32 = jnp.float32
NT = (((1,), (1,)), ((), ()))
TN = (((0,), (0,)), ((), ()))


def mm(a, b):
    return jnp.dot(a, b, preferred_element_type=F32)


def split(x):
    hi = x.astype(BF)
    return hi, (x - hi.astype(F32)).astype(BF)


def iota(shape, axis):
    return lax.broadcasted_iota(jnp.int32, shape, axis)


def core_kernel(
    tok_ref, w_ref, up_ref, floor_ref, rate_ref, diag_ref, gain_ref, out_ref,
    eq_s, wp_s, qe_s, kend_s, cv_s, own_s, decay_s, diag_s, t_s, b_s, state_s, y_s,
):
    length, chans = out_ref.shape
    heads = chans // HEAD
    rank = up_ref.shape[1]
    rows = min(256, length)
    spans = rows // SPAN
    blocks = length // SPAN

    def head_ones():
        return (iota((chans, chans), 0) // HEAD == iota((chans, chans), 1) // HEAD).astype(BF)

    def head_sum(x, ones):
        hi, lo = split(x)
        return mm(hi, ones) + mm(lo, ones)

    @pl.loop(0, length // rows)
    def _(step):
        at = pl.ds(pl.multiple_of(step * rows, rows), rows)
        source = tok_ref[at, :]
        pr = mm(source, w_ref[:, :chans]).astype(BF).astype(F32)
        pk = mm(source, w_ref[:, chans : 2 * chans]).astype(BF).astype(F32)
        pv = mm(source, w_ref[:, 2 * chans : 3 * chans]).astype(BF).astype(F32)
        lowered = jnp.tanh(mm(source, w_ref[:, 3 * chans :])).astype(BF)
        ones = head_ones()
        norm2 = head_sum(pk * pk, ones) + 1.0
        inv = lax.rsqrt(norm2)
        scale = norm2 * inv
        normed = pk * inv
        cv_s[at, :] = scale * pv
        rates = jax.nn.sigmoid(rate_ref[...])
        both = jnp.sum(rates * diag_ref[...], axis=0, keepdims=True)
        own_s[at, :] = head_sum(pr * pk * both, ones) * pv
        ri = iota((rows, rows), 0)
        ci = iota((rows, rows), 1)
        same = ri // SPAN == ci // SPAN
        whole = same.astype(BF)
        for d in range(2):
            pre = (
                mm(lowered[:, d * rank : (d + 1) * rank], up_ref[d]) + floor_ref[d : d + 1, :]
            ).astype(BF).astype(F32)
            fall = -math.exp(-0.5) * jax.nn.sigmoid(pre)
            tri = jnp.logical_and(same, (ci <= ri) if d == 0 else (ci >= ri)).astype(BF)
            hi, lo = split(fall)
            inclusive = mm(tri, hi) + mm(tri, lo)
            final = mm(whole, hi) + mm(whole, lo)
            half = 0.5 * final
            grow = jnp.exp(inclusive - half)
            shrink = jnp.exp(half - inclusive)
            g = jnp.exp(half)
            e = -normed * (grow * jnp.exp(-fall))
            q = pr * grow
            w = normed * rates[d : d + 1, :] * shrink
            wp_s[d, at, :] = w.astype(BF)
            kend_s[d, at, :] = (w * g).astype(BF)
            eb, qb = e.astype(BF), q.astype(BF)
            eg, qg = (e * g).astype(BF), (q * g).astype(BF)
            g2 = g * g
            diag_s[d, at, :] = head_sum(pr * normed * rates[d : d + 1, :], ones)
            for s in range(spans):
                cut = slice(s * SPAN, (s + 1) * SPAN)
                base = pl.multiple_of((step * spans + s) * 2 * SPAN, 2 * SPAN)
                eq_s[d, pl.ds(base, SPAN), :] = eb[cut]
                eq_s[d, pl.ds(base + SPAN, SPAN), :] = qb[cut]
                qe_s[d, pl.ds(base, SPAN), :] = eg[cut]
                qe_s[d, pl.ds(base + SPAN, SPAN), :] = qg[cut]
                decay_s[d, pl.ds(pl.multiple_of((step * spans + s) * 8, 8), 8), :] = g2[
                    s * SPAN : s * SPAN + 8
                ]

    def spread(x, mask):
        x = x.astype(BF)
        if heads > 1:
            x = jnp.concatenate([x] * heads, axis=0)
        return x * mask

    group = 2 if blocks % 2 == 0 else 1

    @pl.loop(0, blocks // group)
    def _(step):
        mask = head_ones()
        ti = iota((SPAN, chans), 0)
        ji = iota((SPAN, chans), 1) % HEAD
        eye = (ti == ji).astype(F32)
        work = []
        for s in range(group):
            for d in range(2):
                block = step * group + s
                two = pl.ds(pl.multiple_of(block * 2 * SPAN, 2 * SPAN), 2 * SPAN)
                at = pl.ds(pl.multiple_of(block * SPAN, SPAN), SPAN)
                ab = lax.dot_general(
                    eq_s[d, two, :], spread(wp_s[d, at, :], mask), NT, preferred_element_type=F32
                )
                strict = (ti > ji) if d == 0 else (ti < ji)
                b_s[d, at, :] = jnp.where(strict, ab[SPAN:], 0.0).astype(BF)
                work.append((d, at, jnp.where(strict, ab[:SPAN], 0.0)))
        near = ti // 4 == ji // 4
        full = [a for _, _, a in work]
        base = [jnp.where(near, a, 0.0) for a in full]
        square = [mm(a.astype(BF), spread(a, mask)) for a in base]
        inverse = [eye + a for a in base]
        inverse = [t + mm(t.astype(BF), spread(a2, mask)) for t, a2 in zip(inverse, square)]
        size = 4
        while size < SPAN:
            far = jnp.logical_and(ti // (2 * size) == ji // (2 * size), ti // size != ji // size)
            first = [
                mm(t.astype(BF), spread(jnp.where(far, a, 0.0), mask))
                for t, a in zip(inverse, full)
            ]
            inverse = [t + mm(f.astype(BF), spread(t, mask)) for t, f in zip(inverse, first)]
            size *= 2
        for (d, at, _), t in zip(work, inverse):
            t_s[d, at, :] = (t - eye).astype(BF)

    state_s[...] = jnp.zeros_like(state_s)

    @pl.loop(0, blocks)
    def _(step):
        mask = head_ones()
        for d in range(2):
            block = step if d == 0 else blocks - 1 - step
            two = pl.ds(pl.multiple_of(block * 2 * SPAN, 2 * SPAN), 2 * SPAN)
            at = pl.ds(pl.multiple_of(block * SPAN, SPAN), SPAN)
            state = state_s[d]
            read = lax.dot_general(
                qe_s[d, two, :], state.astype(BF), NT, preferred_element_type=F32
            )
            x = cv_s[at, :] + read[:SPAN]
            exact = x + mm(t_s[d, at, :], spread(x, mask))
            a = exact.astype(BF)
            y_s[d, at, :] = read[SPAN:] + mm(b_s[d, at, :], spread(a, mask)) + diag_s[d, at, :] * exact
            decay = decay_s[d, pl.ds(pl.multiple_of(block * 8, 8), 8), :][:1]
            put = lax.dot_general(a, kend_s[d, at, :], TN, preferred_element_type=F32)
            state_s[d] = state * decay + put * mask.astype(F32)

    @pl.loop(0, length // rows)
    def _(step):
        at = pl.ds(pl.multiple_of(step * rows, rows), rows)
        ones = head_ones()
        total = own_s[at, :]
        for d in range(2):
            y = y_s[d, at, :]
            centred = y - head_sum(y, ones) * (1.0 / HEAD)
            variance = head_sum(centred * centred, ones) * (1.0 / HEAD)
            total = total + centred * lax.rsqrt(variance + 0.00064) * gain_ref[...]
        out_ref[at, :] = total.astype(BF)


MESH = pl.DeviceIdType.MESH


def whole_kernel(
    sp, dp, tok_ref, w_ref, up_ref, floor_ref, rate_ref, diag_ref, gain_ref, out_ref,
    tok_all, w_all, out_all, slots,
    ring_out, ring_in, far_out, far_in, pass_out, pass_in, back_out, back_in, *scratch,
):
    rows = tok_ref.shape[0]
    half_rows = rows // 2
    depth = w_ref.shape[0]
    chans = out_all.shape[1]
    chips = dp // 2
    z = lax.axis_index("sp")
    me = lax.axis_index("dp")
    chip = me // 2
    core = me % 2
    partner = chip * 2 + 1 - core

    def peer(k):
        return lax.rem(chip + k, chips) * 2 + core

    def z_peer(k):
        return lax.rem(z + k, sp)

    barrier = pltpu.get_barrier_semaphore()
    for target in [(z, partner)] + [(z, peer(k)) for k in range(1, chips)] + [
        (z_peer(k), me) for k in range(1, sp)
    ]:
        pl.semaphore_signal(barrier, inc=1, device_id=target, device_id_type=MESH)
    pl.semaphore_wait(barrier, chips + sp - 1)

    def remote(src, dst, out_sem, in_sem, target):
        copy = pltpu.make_async_remote_copy(
            src_ref=src, dst_ref=dst, send_sem=out_sem, recv_sem=in_sem,
            device_id=target, device_id_type=MESH,
        )
        copy.start()
        return copy

    def w_at(device):
        return pl.ds(pl.multiple_of(device * depth, depth), depth)

    def ring_step(s):
        copies = []
        for way in range(2):
            owner = z_peer(sp - s) if way == 0 else z_peer(s)
            at = pl.ds(
                pl.multiple_of(owner * rows + way * half_rows, half_rows), half_rows
            )
            first = tok_ref.at[pl.ds(way * half_rows, half_rows), :]
            copies.append(
                remote(
                    first if s == 0 else tok_all.at[at, :], tok_all.at[at, :],
                    ring_out.at[way, s], ring_in.at[way, s],
                    (z_peer(1) if way == 0 else z_peer(sp - 1), me),
                )
            )
        return copies

    ring = [ring_step(0)] if sp > 1 else []
    far = [
        remote(w_ref, w_all.at[w_at(me), :], far_out.at[k], far_in.at[k], (z, peer(k)))
        for k in range(1, chips)
    ]
    passed = [remote(w_ref, w_all.at[w_at(me), :], pass_out.at[0], pass_in.at[0], (z, partner))]
    w_all[w_at(me), :] = w_ref[...]
    tok_all[pl.ds(pl.multiple_of(z * rows, rows), rows), :] = tok_ref[...]
    for s in range(max(sp, chips) - 1):
        if s < sp - 1:
            for copy in ring[s]:
                copy.wait_recv()
            if s + 1 < sp - 1:
                ring.append(ring_step(s + 1))
        if s < chips - 1:
            far[s].wait_recv()
            block = w_at(peer(chips - 1 - s))
            passed.append(
                remote(
                    w_all.at[block, :], w_all.at[block, :],
                    pass_out.at[s + 1], pass_in.at[s + 1], (z, partner),
                )
            )
    for copy in passed:
        copy.wait_recv()
    for copy in far + passed + [c for pair in ring for c in pair]:
        copy.wait_send()

    core_kernel(
        tok_all, w_all, up_ref, floor_ref, rate_ref, diag_ref, gain_ref, out_all, *scratch
    )

    def out_at(owner):
        return pl.ds(pl.multiple_of(owner * rows, rows), rows)

    back = [
        remote(
            out_all.at[out_at(z_peer(k)), :], slots.at[z], back_out.at[k], back_in.at[k],
            (z_peer(k), me),
        )
        for k in range(1, sp)
    ]
    slots[z] = out_all[out_at(z), :]
    for copy in back:
        copy.wait()
    for s in range(sp):
        out_ref[:, s * chans : (s + 1) * chans] = slots[s]


def whole_call(sp, dp, rows, depth, chans, width):
    vm = pltpu.VMEM
    dma = pltpu.SemaphoreType.DMA
    length = rows * sp
    both = lambda n, dt: vm((2, n, chans), dt)
    return pl.pallas_call(
        functools.partial(whole_kernel, sp, dp),
        out_shape=jax.ShapeDtypeStruct((rows, chans * sp), BF),
        in_specs=[pl.BlockSpec(memory_space=vm)] * 7,
        out_specs=pl.BlockSpec(memory_space=vm),
        scratch_shapes=[
            vm((length, depth), BF), vm((depth, width), BF), vm((length, chans), BF),
            vm((sp, rows, chans), BF),
            dma((2, sp)), dma((2, sp)), dma((dp,)), dma((dp,)), dma((dp,)), dma((dp,)),
            dma((sp,)), dma((sp,)),
            both(2 * length, BF), both(length, BF), both(2 * length, BF), both(length, BF),
            vm((length, chans), F32), vm((length, chans), F32),
            both(length // SPAN * 8, F32), both(length, F32), both(length, BF), both(length, BF),
            vm((2, chans, chans), F32), both(length, F32),
        ],
        compiler_params=pltpu.CompilerParams(
            vmem_limit_bytes=58 * 1024 * 1024, collective_id=0, has_side_effects=True
        ),
        name="whole",
    )


def per_device(
    sp, dp,
    tokens, receptance_weight, key_projection_weight, value_projection_weight,
    decay_down_weight, decay_up_weight, decay_floor_level, correction_rate_logit,
    diagonal_address_factor, head_norm_gain,
):
    rows, depth = tokens.shape[1:]
    channels = receptance_weight.shape[1]
    chans = channels // sp
    start = lax.axis_index("sp") * chans

    def mine(x):
        return lax.dynamic_slice_in_dim(x, start, chans, axis=x.ndim - 1)

    packed = jnp.concatenate(
        [mine(receptance_weight), mine(key_projection_weight), mine(value_projection_weight),
         decay_down_weight], axis=1)
    mixed = whole_call(sp, dp, rows, depth, chans, packed.shape[1])(
        tokens[0], packed, mine(decay_up_weight), mine(decay_floor_level),
        correction_rate_logit, diagonal_address_factor, head_norm_gain[None, :])
    return mixed[None]


def solution(mesh):
    in_specs = (
        P("dp", "sp", None), P("dp", None), P("dp", None), P("dp", None), P("dp", None),
        P(), P(), P(None, "sp"), P(None, "sp"), P("sp"),
    )
    return jax.shard_map(
        functools.partial(per_device, mesh.shape["sp"], mesh.shape["dp"]), mesh=mesh, in_specs=in_specs,
        out_specs=P("dp", "sp", None), check_vma=False,
    )
```

```python
import functools
import math

import jax
import jax.numpy as jnp
from jax import lax
from jax.experimental import pallas as pl
from jax.experimental.pallas import tpu as pltpu
from jax.sharding import PartitionSpec as P

HEAD = 64
SPAN = 64
BF = jnp.bfloat16
F32 = jnp.float32
NT = (((1,), (1,)), ((), ()))
TN = (((0,), (0,)), ((), ()))


def mm(a, b):
    return jnp.dot(a, b, preferred_element_type=F32)


def split(x):
    hi = x.astype(BF)
    return hi, (x - hi.astype(F32)).astype(BF)


def iota(shape, axis):
    return lax.broadcasted_iota(jnp.int32, shape, axis)


def core_kernel(
    tok_ref, w_ref, up_ref, floor_ref, rate_ref, diag_ref, gain_ref, out_ref,
    eq_s, wp_s, qe_s, kend_s, cv_s, own_s, decay_s, diag_s, t_s, b_s, state_s, y_s,
    arrivals=(),
):
    length, chans = out_ref.shape
    heads = chans // HEAD
    rank = up_ref.shape[1]
    rows = min(256, length)
    blocks = length // SPAN

    def head_ones():
        return (iota((chans, chans), 0) // HEAD == iota((chans, chans), 1) // HEAD).astype(BF)

    def head_sum(x, ones):
        hi, lo = split(x)
        return mm(hi, ones) + mm(lo, ones)

    def at_block(block):
        return pl.ds(pl.multiple_of(block * SPAN, SPAN), SPAN)

    def project(ready):
        tile = SPAN * len(ready)

        def put(ref, x, *lead):
            for s, block in enumerate(ready):
                ref[(*lead, at_block(block), slice(None))] = x[s * SPAN : (s + 1) * SPAN]

        source = jnp.concatenate([tok_ref[at_block(block), :] for block in ready], axis=0)
        pr = mm(source, w_ref[:, :chans]).astype(BF).astype(F32)
        pk = mm(source, w_ref[:, chans : 2 * chans]).astype(BF).astype(F32)
        pv = mm(source, w_ref[:, 2 * chans : 3 * chans]).astype(BF).astype(F32)
        lowered = jnp.tanh(mm(source, w_ref[:, 3 * chans :])).astype(BF)
        ones = head_ones()
        norm2 = head_sum(pk * pk, ones) + 1.0
        inv = lax.rsqrt(norm2)
        scale = norm2 * inv
        normed = pk * inv
        put(cv_s, scale * pv)
        rates = jax.nn.sigmoid(rate_ref[...])
        both = jnp.sum(rates * diag_ref[...], axis=0, keepdims=True)
        put(own_s, head_sum(pr * pk * both, ones) * pv)
        ri = iota((tile, tile), 0)
        ci = iota((tile, tile), 1)
        same = ri // SPAN == ci // SPAN
        whole = same.astype(BF)
        for d in range(2):
            pre = (
                mm(lowered[:, d * rank : (d + 1) * rank], up_ref[d]) + floor_ref[d : d + 1, :]
            ).astype(BF).astype(F32)
            fall = -math.exp(-0.5) * jax.nn.sigmoid(pre)
            tri = jnp.logical_and(same, (ci <= ri) if d == 0 else (ci >= ri)).astype(BF)
            hi, lo = split(fall)
            inclusive = mm(tri, hi) + mm(tri, lo)
            final = mm(whole, hi) + mm(whole, lo)
            half = 0.5 * final
            grow = jnp.exp(inclusive - half)
            shrink = jnp.exp(half - inclusive)
            g = jnp.exp(half)
            e = -normed * (grow * jnp.exp(-fall))
            q = pr * grow
            w = normed * rates[d : d + 1, :] * shrink
            put(wp_s, w.astype(BF), d)
            put(kend_s, (w * g).astype(BF), d)
            eb, qb = e.astype(BF), q.astype(BF)
            eg, qg = (e * g).astype(BF), (q * g).astype(BF)
            g2 = g * g
            put(diag_s, head_sum(pr * normed * rates[d : d + 1, :], ones), d)
            for s, block in enumerate(ready):
                cut = slice(s * SPAN, (s + 1) * SPAN)
                base = pl.multiple_of(block * 2 * SPAN, 2 * SPAN)
                eq_s[d, pl.ds(base, SPAN), :] = eb[cut]
                eq_s[d, pl.ds(base + SPAN, SPAN), :] = qb[cut]
                qe_s[d, pl.ds(base, SPAN), :] = eg[cut]
                qe_s[d, pl.ds(base + SPAN, SPAN), :] = qg[cut]
                decay_s[d, pl.ds(pl.multiple_of(block * 8, 8), 8), :] = g2[
                    s * SPAN : s * SPAN + 8
                ]

    def spread(x, mask):
        x = x.astype(BF)
        if heads > 1:
            x = jnp.concatenate([x] * heads, axis=0)
        return x * mask

    def invert(ready):
        mask = head_ones()
        ti = iota((SPAN, chans), 0)
        ji = iota((SPAN, chans), 1) % HEAD
        eye = (ti == ji).astype(F32)
        work = []
        for block in ready:
            for d in range(2):
                two = pl.ds(pl.multiple_of(block * 2 * SPAN, 2 * SPAN), 2 * SPAN)
                at = pl.ds(pl.multiple_of(block * SPAN, SPAN), SPAN)
                ab = lax.dot_general(
                    eq_s[d, two, :], spread(wp_s[d, at, :], mask), NT, preferred_element_type=F32
                )
                strict = (ti > ji) if d == 0 else (ti < ji)
                b_s[d, at, :] = jnp.where(strict, ab[SPAN:], 0.0).astype(BF)
                work.append((d, at, jnp.where(strict, ab[:SPAN], 0.0)))
        near = ti // 4 == ji // 4
        full = [a for _, _, a in work]
        base = [jnp.where(near, a, 0.0) for a in full]
        square = [mm(a.astype(BF), spread(a, mask)) for a in base]
        inverse = [eye + a for a in base]
        inverse = [t + mm(t.astype(BF), spread(a2, mask)) for t, a2 in zip(inverse, square)]
        size = 4
        while size < SPAN:
            far = jnp.logical_and(ti // (2 * size) == ji // (2 * size), ti // size != ji // size)
            first = [
                mm(t.astype(BF), spread(jnp.where(far, a, 0.0), mask))
                for t, a in zip(inverse, full)
            ]
            inverse = [t + mm(f.astype(BF), spread(t, mask)) for t, f in zip(inverse, first)]
            size *= 2
        for (d, at, _), t in zip(work, inverse):
            t_s[d, at, :] = (t - eye).astype(BF)

    for settle, ready in arrivals:
        settle()
        project(ready)
        invert(ready)

    state_s[...] = jnp.zeros_like(state_s)

    @pl.loop(0, blocks)
    def _(step):
        mask = head_ones()
        for d in range(2):
            block = step if d == 0 else blocks - 1 - step
            two = pl.ds(pl.multiple_of(block * 2 * SPAN, 2 * SPAN), 2 * SPAN)
            at = pl.ds(pl.multiple_of(block * SPAN, SPAN), SPAN)
            state = state_s[d]
            read = lax.dot_general(
                qe_s[d, two, :], state.astype(BF), NT, preferred_element_type=F32
            )
            x = cv_s[at, :] + read[:SPAN]
            exact = x + mm(t_s[d, at, :], spread(x, mask))
            a = exact.astype(BF)
            y_s[d, at, :] = read[SPAN:] + mm(b_s[d, at, :], spread(a, mask)) + diag_s[d, at, :] * exact
            decay = decay_s[d, pl.ds(pl.multiple_of(block * 8, 8), 8), :][:1]
            put = lax.dot_general(a, kend_s[d, at, :], TN, preferred_element_type=F32)
            state_s[d] = state * decay + put * mask.astype(F32)

    @pl.loop(0, length // rows)
    def _(step):
        at = pl.ds(pl.multiple_of(step * rows, rows), rows)
        ones = head_ones()
        total = own_s[at, :]
        for d in range(2):
            y = y_s[d, at, :]
            centred = y - head_sum(y, ones) * (1.0 / HEAD)
            variance = head_sum(centred * centred, ones) * (1.0 / HEAD)
            total = total + centred * lax.rsqrt(variance + 0.00064) * gain_ref[...]
        out_ref[at, :] = total.astype(BF)


MESH = pl.DeviceIdType.MESH


def whole_kernel(
    sp, dp, tok_ref, w_ref, up_ref, floor_ref, rate_ref, diag_ref, gain_ref, out_ref,
    tok_all, w_all, out_all, slots,
    ring_out, ring_in, far_out, far_in, pass_out, pass_in, back_out, back_in, *scratch,
):
    rows = tok_ref.shape[0]
    half_rows = rows // 2
    depth = w_ref.shape[0]
    chans = out_all.shape[1]
    chips = dp // 2
    z = lax.axis_index("sp")
    me = lax.axis_index("dp")
    chip = me // 2
    core = me % 2
    partner = chip * 2 + 1 - core

    def peer(k):
        return lax.rem(chip + k, chips) * 2 + core

    def z_peer(k):
        return lax.rem(z + k, sp)

    barrier = pltpu.get_barrier_semaphore()
    for target in [(z, partner)] + [(z, peer(k)) for k in range(1, chips)] + [
        (z_peer(k), me) for k in range(1, sp)
    ]:
        pl.semaphore_signal(barrier, inc=1, device_id=target, device_id_type=MESH)
    pl.semaphore_wait(barrier, chips + sp - 1)

    def remote(src, dst, out_sem, in_sem, target):
        copy = pltpu.make_async_remote_copy(
            src_ref=src, dst_ref=dst, send_sem=out_sem, recv_sem=in_sem,
            device_id=target, device_id_type=MESH,
        )
        copy.start()
        return copy

    def w_at(device):
        return pl.ds(pl.multiple_of(device * depth, depth), depth)

    def ring_step(s):
        copies = []
        for way in range(2):
            owner = z_peer(sp - s) if way == 0 else z_peer(s)
            at = pl.ds(
                pl.multiple_of(owner * rows + way * half_rows, half_rows), half_rows
            )
            first = tok_ref.at[pl.ds(way * half_rows, half_rows), :]
            copies.append(
                remote(
                    first if s == 0 else tok_all.at[at, :], tok_all.at[at, :],
                    ring_out.at[way, s], ring_in.at[way, s],
                    (z_peer(1) if way == 0 else z_peer(sp - 1), me),
                )
            )
        return copies

    ring = [ring_step(0)] if sp > 1 else []
    far = [
        remote(w_ref, w_all.at[w_at(me), :], far_out.at[k], far_in.at[k], (z, peer(k)))
        for k in range(1, chips)
    ]
    passed = [remote(w_ref, w_all.at[w_at(me), :], pass_out.at[0], pass_in.at[0], (z, partner))]
    w_all[w_at(me), :] = w_ref[...]
    tok_all[pl.ds(pl.multiple_of(z * rows, rows), rows), :] = tok_ref[...]
    for s in range(max(sp, chips) - 1):
        if s < sp - 2:
            for copy in ring[s]:
                copy.wait_recv()
            ring.append(ring_step(s + 1))
        if s < chips - 1:
            far[s].wait_recv()
            block = w_at(peer(chips - 1 - s))
            passed.append(
                remote(
                    w_all.at[block, :], w_all.at[block, :],
                    pass_out.at[s + 1], pass_in.at[s + 1], (z, partner),
                )
            )
    for copy in passed:
        copy.wait_recv()

    def last_ring():
        for copy in ring[-1]:
            copy.wait_recv()

    per = rows // SPAN
    arrivals = [(lambda: None, [z * per + b for b in range(per)])]
    for s in range(sp - 1):
        before, after = z_peer(sp - 1 - s), z_peer(s + 1)
        ready = [before * per + b for b in range(per // 2)]
        ready += [after * per + b for b in range(per // 2, per)]
        arrivals.append((last_ring if s == sp - 2 else lambda: None, ready))

    core_kernel(
        tok_all, w_all, up_ref, floor_ref, rate_ref, diag_ref, gain_ref, out_all, *scratch,
        arrivals=arrivals,
    )
    for copy in far + passed + [c for pair in ring for c in pair]:
        copy.wait_send()

    def out_at(owner):
        return pl.ds(pl.multiple_of(owner * rows, rows), rows)

    back = [
        remote(
            out_all.at[out_at(z_peer(k)), :], slots.at[z], back_out.at[k], back_in.at[k],
            (z_peer(k), me),
        )
        for k in range(1, sp)
    ]
    slots[z] = out_all[out_at(z), :]
    for copy in back:
        copy.wait()
    for s in range(sp):
        out_ref[:, s * chans : (s + 1) * chans] = slots[s]


def whole_call(sp, dp, rows, depth, chans, width):
    vm = pltpu.VMEM
    dma = pltpu.SemaphoreType.DMA
    length = rows * sp
    both = lambda n, dt: vm((2, n, chans), dt)
    return pl.pallas_call(
        functools.partial(whole_kernel, sp, dp),
        out_shape=jax.ShapeDtypeStruct((rows, chans * sp), BF),
        in_specs=[pl.BlockSpec(memory_space=vm)] * 7,
        out_specs=pl.BlockSpec(memory_space=vm),
        scratch_shapes=[
            vm((length, depth), BF), vm((depth, width), BF), vm((length, chans), BF),
            vm((sp, rows, chans), BF),
            dma((2, sp)), dma((2, sp)), dma((dp,)), dma((dp,)), dma((dp,)), dma((dp,)),
            dma((sp,)), dma((sp,)),
            both(2 * length, BF), both(length, BF), both(2 * length, BF), both(length, BF),
            vm((length, chans), F32), vm((length, chans), F32),
            both(length // SPAN * 8, F32), both(length, F32), both(length, BF), both(length, BF),
            vm((2, chans, chans), F32), both(length, F32),
        ],
        compiler_params=pltpu.CompilerParams(
            vmem_limit_bytes=58 * 1024 * 1024, collective_id=0, has_side_effects=True
        ),
        name="whole",
    )


def per_device(
    sp, dp,
    tokens, receptance_weight, key_projection_weight, value_projection_weight,
    decay_down_weight, decay_up_weight, decay_floor_level, correction_rate_logit,
    diagonal_address_factor, head_norm_gain,
):
    rows, depth = tokens.shape[1:]
    channels = receptance_weight.shape[1]
    chans = channels // sp
    start = lax.axis_index("sp") * chans

    def mine(x):
        return lax.dynamic_slice_in_dim(x, start, chans, axis=x.ndim - 1)

    packed = jnp.concatenate(
        [mine(receptance_weight), mine(key_projection_weight), mine(value_projection_weight),
         decay_down_weight], axis=1)
    mixed = whole_call(sp, dp, rows, depth, chans, packed.shape[1])(
        tokens[0], packed, mine(decay_up_weight), mine(decay_floor_level),
        correction_rate_logit, diagonal_address_factor, head_norm_gain[None, :])
    return mixed[None]


def solution(mesh):
    in_specs = (
        P("dp", "sp", None), P("dp", None), P("dp", None), P("dp", None), P("dp", None),
        P(), P(), P(None, "sp"), P(None, "sp"), P("sp"),
    )
    return jax.shard_map(
        functools.partial(per_device, mesh.shape["sp"], mesh.shape["dp"]), mesh=mesh, in_specs=in_specs,
        out_specs=P("dp", "sp", None), check_vma=False,
    )
```
